512 devices in a mesh: fs: 128 (over z, x, core), tp: 4 (over y).
Axes of the slice: x: 4, y: 4, z: 16, core: 2. Of those that a mesh axis runs over, the one named last changes fastest.
Arguments:
- tokens: bfloat16 [16384, 2048], P('fs', 'tp'), may hold values from -6 to 6
- routes: int32 [16384, 2], P('fs'), may hold values from 0 to 63, all different within a row; in each aligned block of 128 rows (0 to 127, 128 to 255, ...) at most 6 rows name the same one
- route_weight: float32 [16384, 2], P('fs'), may hold values from 0.1 to 1
- norm_gain: float32 [2048], P('fs'), may hold values from 0.1 to 1.9
- expert_gate: float32 [64, 2048, 512], P(None, 'fs', 'tp'), may hold values from -0.125 to 0.125
- expert_up: float32 [64, 2048, 512], P(None, 'fs', 'tp'), may hold values from -0.125 to 0.125
- expert_down: float32 [64, 2048, 512], P(None, 'fs', 'tp'), may hold values from -0.25 to 0.25
- shared_gate: float32 [2048, 512], P('fs', 'tp'), may hold values from -0.125 to 0.125
- shared_up: float32 [2048, 512], P('fs', 'tp'), may hold values from -0.125 to 0.125
- shared_down: float32 [512, 2048], P('tp', 'fs'), may hold values from -0.25 to 0.25
Outputs:
- mixed: bfloat16 [16384, 2048], P('fs', 'tp')
- gate_sampler: bfloat16 [128, 2048, 256], P('fs', None, 'tp')
- up_sampler: bfloat16 [128, 2048, 256], P('fs', None, 'tp')
- down_sampler: bfloat16 [128, 2048, 256], P('fs', 'tp')
- shared_gate_out: bfloat16 [2048, 512], P(None, 'tp')
- shared_up_out: bfloat16 [2048, 512], P(None, 'tp')
- shared_down_out: bfloat16 [512, 2048], P('tp')
The draws below stay inside these ranges and needn't reach their ends.
Inputs may be any that keep to these rules, and one draw needn't show every extreme that they name: `routes`: each row names 2 different experts. In each aligned block of 128 rows no expert is named by more than 6 rows, a bound that some block reaches.
All inputs are finite; a program needn't handle non-finite values.
Results may differ from the reference program's by a relative error of at most 0.009.
Values may be sent and summed in bfloat16 or wider, within the bound.
A program may use at most 64 MiB of HBM per device.

```python
import math
import jax
import jax.numpy as jnp
import numpy as np
from jax import lax

D = 2048
FF = 512
TOP_K = 2
TOK_DEV = 128
EXPERTS = 64
UNITS = 64
SHARED_BLOCK = 128
CAP = 6
TOKENS = 16384
N_FS = 128
N_TP = 4


def steps_of(rng, shape, split, least, high):
    gain = 1.0
    for dim, blocks in split:
        heights = jax.random.uniform(jax.random.fold_in(jax.random.fold_in(rng, 6), dim), (blocks,), jnp.float32, least / len(split), high / len(split))
        gain = gain * jnp.repeat(jnp.exp(heights), shape[dim] // blocks).reshape((-1,) + (1,) * (len(shape) - 1 - dim))
    return gain


def routed_block(own_key, own, number, rows, number_of, top, most, slope):
    sequence = jax.random.permutation(own_key, number_of)
    heavy_load, ordinary = shares(number_of, rows * top, most, slope, True), shares(number_of, rows * top, most, slope, False)
    places = jnp.arange(number_of)

    def named(sizes, turn):
        used = int((sizes > 0).sum())
        fixed = max(1, used // 4)
        passed = fixed + (places - fixed + turn * (used - fixed)) % max(1, number_of - fixed)
        return jnp.zeros((number_of,), jnp.int32).at[sequence[jnp.where(places < fixed, places, passed)]].set(jnp.asarray(sizes, jnp.int32))

    sizes = jnp.where(number % 4 == 0, named(heavy_load, number // 4), named(ordinary, number - number // 4 - 1))
    mixed = jax.random.permutation(jax.random.fold_in(own, 3), number_of)
    giver, sink = mixed[0:number_of // 2 * 2:2], mixed[1:number_of // 2 * 2:2]
    margin = jnp.minimum(sizes[giver] - 1, most - sizes[sink]) // 2
    margin = jnp.where((giver == sequence[0]) | (sink == sequence[0]) | (sizes[sink] == 0), 0, jnp.maximum(margin, 0))
    passed = jax.random.randint(jax.random.fold_in(own, 4), (number_of // 2,), 0, 1 << 20) % (margin + 1)
    sizes = sizes.at[giver].add(-passed).at[sink].add(passed)
    items = jnp.searchsorted(jnp.cumsum(sizes), jnp.arange(rows * top), side="right").astype(jnp.int32)
    table = items.reshape(top, rows).T
    table = table[jax.random.permutation(jax.random.fold_in(own, 1), rows)]
    turn = jax.random.randint(jax.random.fold_in(own, 2), (rows, 1), 0, top)
    return jnp.take_along_axis(table, (jnp.arange(top)[None, :] + turn) % top, axis=1)


def shares(amount, total, limit, lean, full):
    portions = [(1 << 20) // math.isqrt(rank ** lean) + 1 for rank in range(1, amount + 1)]
    largest = limit if full else min(limit, max(-(-total // amount), total * portions[0] // sum(portions)))
    least = 1 if total - largest >= amount - 1 else 0
    given, rest = [largest] + [least] * (amount - 1), total - largest - least * (amount - 1)
    while rest > 0:
        movable = [i for i in range(1, amount) if given[i] < largest] or [i for i in range(1, amount) if given[i] < limit]
        mass, budget = sum([portions[i] for i in movable]), rest
        for i in movable:
            addition = min(limit - given[i], max(1, budget * portions[i] // mass), rest)
            given[i] = given[i] + addition
            rest = rest - addition
    return np.array(given)


def noise(stream_key, extent, width, bound, pieces=(), held_as=jnp.bfloat16):
    gain = steps_of(stream_key, extent, pieces, -0.22, 0.18) if pieces else 1.0
    values = jax.random.normal(stream_key, extent, jnp.float32) * width * gain
    return jnp.minimum(jnp.maximum(values, -bound), bound).astype(held_as)


def setup_inputs(seed: int = 0) -> dict:
    keys = jax.random.split(jax.random.key(seed), 11)
    tokens = noise(keys[0], (TOKENS, D), 1.0, 6.0, ((0, 128), (1, 4)))
    routes_keys = jax.random.split(jax.random.fold_in(keys[1], 1), TOKENS // TOK_DEV)
    routes_turns = jax.random.permutation(jax.random.fold_in(keys[1], 3), TOKENS // TOK_DEV)
    routes = jax.vmap(lambda own, number: routed_block(jax.random.fold_in(keys[1], 2), own, number, TOK_DEV, EXPERTS, TOP_K, CAP, 0))(routes_keys, routes_turns).reshape((TOKENS, TOP_K))
    route_weight = jnp.clip(0.1 + 0.9 * jax.random.uniform(keys[2], (TOKENS, TOP_K), jnp.float32) ** steps_of(keys[2], (TOKENS, TOP_K), ((0, 128),), -0.2, 0.2), 0.1, 1.0)
    norm_gain = jnp.clip(1.0 + 0.18 * jax.random.normal(keys[3], (D,), jnp.float32), 0.1, 1.9)
    expert_gate = noise(keys[4], (EXPERTS, D, FF), D ** -0.5, 0.125, ((1, 128), (2, 4)), jnp.float32)
    expert_up = noise(keys[5], (EXPERTS, D, FF), D ** -0.5, 0.125, ((1, 128), (2, 4)), jnp.float32)
    expert_down = noise(keys[6], (EXPERTS, D, FF), FF ** -0.5, 0.25, ((1, 128), (2, 4)), jnp.float32)
    shared_gate = noise(keys[7], (D, FF), D ** -0.5, 0.125, ((0, 128), (1, 4)), jnp.float32)
    shared_up = noise(keys[8], (D, FF), D ** -0.5, 0.125, ((0, 128), (1, 4)), jnp.float32)
    shared_down = noise(keys[9], (FF, D), FF ** -0.5, 0.25, ((0, 4), (1, 128)), jnp.float32)
    return {"tokens": tokens, "routes": routes, "route_weight": route_weight, "norm_gain": norm_gain, "expert_gate": expert_gate, "expert_up": expert_up, "expert_down": expert_down, "shared_gate": shared_gate, "shared_up": shared_up, "shared_down": shared_down}


EPS = 1e-06

def slot_places(routes):
    blocks = routes.reshape(N_FS, TOK_DEV * TOP_K)
    onehot = (blocks[:, :, None] == jnp.arange(EXPERTS, dtype=jnp.int32)[None, None, :]).astype(jnp.int32)
    earlier = jnp.cumsum(onehot, axis=1) - onehot
    position = lax.optimization_barrier(jnp.sum(earlier * onehot, axis=2))
    return (blocks * CAP + position).astype(jnp.int32)

def to_sampler(folded):
    return folded.reshape(EXPERTS, D, N_TP, 2, UNITS).transpose(0, 3, 1, 2, 4).reshape(2 * EXPERTS, D, N_TP * UNITS)

def reference(tokens, routes, route_weight, norm_gain, expert_gate, expert_up, expert_down, shared_gate, shared_up, shared_down):
    gate_folded = (expert_gate * norm_gain[None, :, None]).astype(jnp.bfloat16)
    up_folded = (expert_up * norm_gain[None, :, None]).astype(jnp.bfloat16)
    down_round = expert_down.astype(jnp.bfloat16)
    gate_sampler = to_sampler(gate_folded)
    up_sampler = to_sampler(up_folded)
    down_sampler = to_sampler(down_round)
    shared_gate_out = (shared_gate * norm_gain[:, None]).astype(jnp.bfloat16)
    shared_up_out = (shared_up * norm_gain[:, None]).astype(jnp.bfloat16)
    shared_down_out = shared_down.astype(jnp.bfloat16)
    tokens_wide = tokens.astype(jnp.float32)
    normed = (tokens_wide * lax.rsqrt(lax.optimization_barrier(jnp.mean(tokens_wide * tokens_wide, axis=1, keepdims=True)) + EPS)).astype(jnp.bfloat16)
    shared_act = jnp.dot(normed, shared_gate_out, preferred_element_type=jnp.float32)
    shared_lin = jnp.dot(normed, shared_up_out, preferred_element_type=jnp.float32)
    shared_hidden = (jax.nn.silu(shared_act) * shared_lin).astype(jnp.bfloat16)
    shared_sum = jnp.zeros((TOKENS, D), jnp.float32)
    for tp_part in range(N_TP):
        lower = tp_part * SHARED_BLOCK
        product = jnp.dot(shared_hidden[:, lower:lower + SHARED_BLOCK], shared_down_out[lower:lower + SHARED_BLOCK], preferred_element_type=jnp.float32)
        shared_sum = shared_sum + lax.optimization_barrier(product.astype(jnp.bfloat16)).astype(jnp.float32)
    places = slot_places(routes)
    block_ids = jnp.arange(N_FS, dtype=jnp.int32)[:, None]
    token_ids = (block_ids * TOK_DEV + jnp.arange(TOK_DEV * TOP_K, dtype=jnp.int32)[None, :] // TOP_K).astype(jnp.int32)
    slot_table = jnp.full((N_FS, EXPERTS * CAP), TOKENS, jnp.int32).at[block_ids, places].set(token_ids)
    slot_weight = jnp.zeros((N_FS, EXPERTS * CAP), jnp.float32).at[block_ids, places].set(route_weight.reshape(N_FS, TOK_DEV * TOP_K))
    slot_table = slot_table.reshape(N_FS, EXPERTS, CAP).transpose(1, 0, 2).reshape(EXPERTS, N_FS * CAP)
    slot_weight = slot_weight.reshape(N_FS, EXPERTS, CAP).transpose(1, 0, 2).reshape(EXPERTS, N_FS * CAP)
    padded = jnp.concatenate([normed, jnp.zeros((1, D), jnp.bfloat16)], axis=0)

    def expert_step(totals, inputs):
        row_ids, weights, gate_rows, up_rows, down_rows = inputs
        picked = padded[row_ids]
        gate_act = jnp.dot(picked, gate_rows, preferred_element_type=jnp.float32)
        up_act = jnp.dot(picked, up_rows, preferred_element_type=jnp.float32)
        hidden = (jax.nn.silu(gate_act) * up_act).astype(jnp.bfloat16).reshape(N_FS * CAP, N_TP, 2, UNITS)
        down_parts = down_rows.reshape(D, N_TP, 2, UNITS)
        combined = jnp.zeros((N_FS * CAP, D), jnp.float32)
        for half_index in range(2):
            down_half = down_parts[:, :, half_index, :].reshape(D, N_TP * UNITS)
            product = jnp.dot(hidden[:, :, half_index, :].reshape(N_FS * CAP, N_TP * UNITS), down_half.T, preferred_element_type=jnp.float32)
            combined = combined + lax.optimization_barrier(product.astype(jnp.bfloat16)).astype(jnp.float32)
        return (totals.at[row_ids].add(combined * weights[:, None]), None)
    routed_total, _ = lax.scan(expert_step, jnp.zeros((TOKENS + 1, D), jnp.float32), (slot_table, slot_weight, gate_folded, up_folded, down_round))
    mixed = (shared_sum + routed_total[:TOKENS]).astype(jnp.bfloat16)
    return (mixed, gate_sampler, up_sampler, down_sampler, shared_gate_out, shared_up_out, shared_down_out)
```

```python
import functools

import jax
import jax.numpy as jnp
import numpy as np
from jax import lax
from jax.experimental import pallas as pl
from jax.experimental.pallas import tpu as pltpu
from jax.sharding import Mesh
from jax.sharding import PartitionSpec as P

FS = ("z", "x", "c")
EPS = 1e-06
MESH = pl.DeviceIdType.MESH
BF = jnp.bfloat16
F32 = jnp.float32
CAP = 6
LANES = 128


def turn_matrix():
    turn = np.zeros((8 * 4 * CAP, 8 * 4 * CAP), np.float32)
    for block in range(4):
        for source in range(8):
            for slot in range(CAP):
                turn[block * 8 * CAP + source * CAP + slot, source * 4 * CAP + block * CAP + slot] = 1
    return turn


def peer_at(step, z, x, zs, xs):
    pair = step // xs
    dz = pair // 2 + 1 - (zs // 2) * (pair % 2)
    dx = (step % xs + 1) % xs
    return lax.rem(z + dz + zs, zs), lax.rem(x + dx, xs)


def await_bytes(ref, sem):
    pltpu.make_async_copy(ref, ref, sem).wait()


def kernel(
    zs, xs, ys,
    tok, route, weight, gain, gate, up, down, s_gate, s_up, s_down, turn, turn_back,
    mixed, gate_out, up_out, down_out, sg_out, su_out, sd_out,
    tok_src, gu_src, down_src, tok_in, gu, down_in, dd, sh, own_tok, rows, normed, hid,
    part_src, part_in, back_src, back_in,
    send, recv, tok_sem, row_sem, hid_sem,
):
    z, x, c, y = (lax.axis_index(a) for a in ("z", "x", "c", "y"))
    me = z * xs + x
    others = zs * xs - 1
    above, below = lax.rem(y + 1, ys), lax.rem(y + ys - 1, ys)
    far = lax.rem(y + 2, ys)

    barrier = pltpu.get_barrier_semaphore()

    def greet(step, carry):
        pz, px = peer_at(step, z, x, zs, xs)
        pl.semaphore_signal(barrier, inc=1, device_id={"z": pz, "x": px}, device_id_type=MESH)
        return carry

    lax.fori_loop(0, others, greet, 0)
    for k in range(1, ys):
        pl.semaphore_signal(
            barrier, inc=1, device_id={"y": lax.rem(y + k, ys)}, device_id_type=MESH
        )
    pl.semaphore_signal(barrier, inc=1, device_id={"c": 1 - c}, device_id_type=MESH)

    experts = zs * xs
    slab = 4 * CAP
    shape = (experts, slab, LANES)
    expert_id = lax.broadcasted_iota(jnp.int32, shape, 0)
    place = lax.broadcasted_iota(jnp.int32, shape, 1)
    block = (
        (place >= CAP).astype(jnp.int32)
        + (place >= 2 * CAP).astype(jnp.int32)
        + (place >= 3 * CAP).astype(jnp.int32)
    )
    slot = place - CAP * block
    first = route[0:1, :].reshape(1, 1, LANES) == expert_id
    second = route[1:2, :].reshape(1, 1, LANES) == expert_id
    named = (first | second).astype(F32).reshape(experts * slab, LANES)
    before = (
        lax.broadcasted_iota(jnp.int32, (LANES, LANES), 0)
        < lax.broadcasted_iota(jnp.int32, (LANES, LANES), 1)
    ).astype(BF)
    position = jnp.dot(named.astype(BF), before, preferred_element_type=F32)
    slot_f = slot.astype(F32).reshape(experts * slab, LANES)
    picked = jnp.where(position == slot_f, named, 0.0)
    chosen = jnp.dot(picked.astype(BF), tok[...], preferred_element_type=F32)
    block_2d = block.reshape(experts * slab, LANES)
    packed = chosen[:, 0:LANES]
    for k in range(1, 4):
        packed = jnp.where(block_2d == k, chosen[:, k * LANES : (k + 1) * LANES], packed)
    tok_src[...] = packed.astype(BF).reshape(shape)
    scale = gain[...][None]
    gu_src[:, 0] = (gate[...] * scale).astype(BF)
    gu_src[:, 1] = (up[...] * scale).astype(BF)
    down_src[...] = down[...].astype(BF)
    sh[me, c, 0] = (s_gate[...] * gain[...]).astype(BF)
    sh[me, c, 1] = (s_up[...] * gain[...]).astype(BF)
    sh[me, c, 2] = s_down[...].astype(BF)
    own_tok[y] = tok[...]
    tok_in[me] = tok_src[me]
    gu[me, c] = gu_src[me]
    down_in[me] = down_src[me]

    pl.semaphore_wait(barrier, others + ys)

    def remote(src, dst, send_sem, recv_sem, to):
        return pltpu.make_async_remote_copy(
            src_ref=src, dst_ref=dst, send_sem=send_sem, recv_sem=recv_sem,
            device_id=to, device_id_type=MESH,
        )

    def ring_start(buf, sems):
        remote(buf.at[y], buf.at[y], sems.at[0], sems.at[4], {"y": above}).start()
        remote(buf.at[y], buf.at[y], sems.at[1], sems.at[5], {"y": below}).start()

    def ring_forward(buf, sems):
        half = buf.shape[1] // 2
        await_bytes(buf.at[below], sems.at[4])
        low = buf.at[below, pl.ds(0, half)]
        remote(low, low, sems.at[2], sems.at[6], {"y": above}).start()
        await_bytes(buf.at[above], sems.at[5])
        high = buf.at[above, pl.ds(half, half)]
        remote(high, high, sems.at[3], sems.at[7], {"y": below}).start()

    def ring_finish(buf, sems):
        half = buf.shape[1] // 2
        await_bytes(buf.at[far, pl.ds(0, half)], sems.at[6])
        await_bytes(buf.at[far, pl.ds(half, half)], sems.at[7])

    def ring_drain(buf, sems):
        half = buf.shape[1] // 2
        await_bytes(buf.at[y], sems.at[0])
        await_bytes(buf.at[y], sems.at[1])
        await_bytes(buf.at[y, pl.ds(0, half)], sems.at[2])
        await_bytes(buf.at[y, pl.ds(0, half)], sems.at[3])

    def to_columns(src_at, dst_at, number):
        def one(step, carry):
            pz, px = peer_at(step, z, x, zs, xs)
            remote(
                src_at(pz * xs + px), dst_at, send.at[number], recv.at[number],
                {"z": pz, "x": px},
            ).start()
            return carry

        lax.fori_loop(0, others, one, 0)

    quarter = zs // 4
    for k in range(1, 4):
        pz = lax.rem(z + k * quarter, zs)
        remote(sh.at[me, c], sh.at[me, c], send.at[0], recv.at[0], {"z": pz}).start()
    ring_start(own_tok, tok_sem)
    to_columns(lambda e: tok_src.at[e], tok_in.at[me], 1)
    await_bytes(sh.at[pl.ds(0, 3), c], recv.at[0])
    for k in range(1, quarter):
        pz = lax.rem(z - z % quarter + (z + k) % quarter, zs)
        for q in range(4):
            piece = (z % quarter + q * quarter) * xs + x
            remote(sh.at[piece, c], sh.at[piece, c], send.at[2], recv.at[2], {"z": pz}).start()
    to_columns(lambda e: gu_src.at[e], gu.at[me, c], 3)
    to_columns(lambda e: down_src.at[e], down_in.at[me], 4)
    ring_forward(own_tok, tok_sem)

    await_bytes(tok_in.at[pl.ds(0, others)], recv.at[1])
    group = 8 * CAP
    for g in range(experts // 8):
        lines = tok_in[pl.ds(8 * g, 8)].reshape(8 * slab, LANES)
        turned = jnp.dot(turn[...], lines, preferred_element_type=F32).astype(BF)
        for k in range(4):
            rows[y, pl.ds(g * group, group), pl.ds(k * LANES, LANES)] = turned[
                k * group : (k + 1) * group
            ]
    ring_start(rows, row_sem)

    await_bytes(sh.at[pl.ds(0, 4 * (quarter - 1)), c], recv.at[2])

    def spread(step, carry):
        piece = step * xs + x
        for k in range(1, xs):
            px = lax.rem(x + k, xs)
            remote(sh.at[piece, c], sh.at[piece, c], send.at[5], recv.at[5], {"x": px}).start()
        return carry

    lax.fori_loop(0, zs, spread, 0)

    ring_finish(own_tok, tok_sem)
    wide = [own_tok[k].astype(F32) for k in range(ys)]
    total = sum(jnp.sum(w * w, axis=1, keepdims=True) for w in wide)
    factor = lax.rsqrt(total * (1.0 / (ys * tok.shape[1])) + EPS)
    own_normed = [(w * factor).astype(BF) for w in wide]

    ring_forward(rows, row_sem)

    await_bytes(sh.at[pl.ds(0, (xs - 1) * zs), c], recv.at[5])
    remote(sh.at[:, c], sh.at[:, c], send.at[6], recv.at[6], {"c": 1 - c}).start()

    ring_finish(rows, row_sem)
    row_total = jnp.zeros((rows.shape[1], 1), F32)
    for k in range(ys):
        part = rows[k].astype(F32)
        row_total = row_total + jnp.sum(part * part, axis=1, keepdims=True)
    row_factor = lax.rsqrt(row_total * (1.0 / (ys * tok.shape[1])) + EPS)
    for k in range(ys):
        normed[k] = (rows[k].astype(F32) * row_factor).astype(BF)

    share = experts // ys
    await_bytes(sh.at[:, c], recv.at[6])

    def stacked(ref, k, number):
        return ref[pl.ds(k * share, share), :, number].reshape(share * 2 * 16, LANES)

    act = sum(
        jnp.dot(own_normed[k], stacked(sh, k, 0), preferred_element_type=F32) for k in range(ys)
    )
    lin = sum(
        jnp.dot(own_normed[k], stacked(sh, k, 1), preferred_element_type=F32) for k in range(ys)
    )
    shared_hidden = (act / (1.0 + jnp.exp(-act)) * lin).astype(BF)
    nt = (((1,), (1,)), ((), ()))
    for k in range(ys):
        part_src[k] = lax.dot_general(
            shared_hidden, stacked(sh, k, 2), nt, preferred_element_type=F32
        ).astype(BF)
    part_in[y] = part_src[y]
    for k in range(1, ys):
        to = lax.rem(y + k, ys)
        remote(part_src.at[to], part_in.at[y], send.at[7], recv.at[7], {"y": to}).start()

    await_bytes(gu.at[pl.ds(0, others), c], recv.at[3])
    remote(gu.at[:, c], gu.at[:, c], send.at[8], recv.at[8], {"c": 1 - c}).start()
    await_bytes(gu.at[:, c], recv.at[8])
    act = sum(
        jnp.dot(normed[k], stacked(gu, k, 0), preferred_element_type=F32) for k in range(ys)
    )
    lin = sum(
        jnp.dot(normed[k], stacked(gu, k, 1), preferred_element_type=F32) for k in range(ys)
    )
    hid[y] = (act / (1.0 + jnp.exp(-act)) * lin).astype(BF)
    ring_start(hid, hid_sem)

    await_bytes(down_in.at[pl.ds(0, others)], recv.at[4])
    dd[pl.ds(y * share, share), c] = down_in[pl.ds(y * share, share)]
    for k in range(1, ys):
        to = lax.rem(y + k, ys)
        remote(
            down_in.at[pl.ds(to * share, share)], dd.at[pl.ds(y * share, share), c],
            send.at[9], recv.at[9], {"y": to},
        ).start()
    ring_forward(hid, hid_sem)
    await_bytes(dd.at[pl.ds(0, (ys - 1) * share), c], recv.at[9])
    remote(dd.at[:, c], dd.at[:, c], send.at[10], recv.at[10], {"c": 1 - c}).start()
    ring_finish(hid, hid_sem)
    await_bytes(dd.at[:, c], recv.at[10])
    result = sum(
        lax.dot_general(
            hid[k], dd[pl.ds(k * share, share)].reshape(share * 2 * 16, LANES), nt,
            preferred_element_type=F32,
        )
        for k in range(ys)
    ).astype(BF)
    for g in range(experts // 8):
        part = result[g * group : (g + 1) * group]
        lines = jnp.concatenate([part[:, k * LANES : (k + 1) * LANES] for k in range(4)], axis=0)
        turned = jnp.dot(turn_back[...], lines, preferred_element_type=F32).astype(BF)
        back_src[pl.ds(8 * g, 8)] = turned.reshape(8, slab, LANES)
    back_in[me] = back_src[me]
    to_columns(lambda e: back_src.at[e], back_in.at[me], 11)

    half_rows = lax.broadcasted_iota(jnp.int32, (64, LANES), 0) + 64 * c
    pick = (half_rows == lax.broadcasted_iota(jnp.int32, (64, LANES), 1)).astype(BF)
    same = (
        lax.broadcasted_iota(jnp.int32, (LANES, LANES), 0)
        == lax.broadcasted_iota(jnp.int32, (LANES, LANES), 1)
    ).astype(BF)
    wide_share = share * 2 * 16
    for k in range(ys):
        cols = pl.ds(k * wide_share, wide_share)
        gate_out[0, :, cols] = lax.dot_general(
            pick, stacked(gu, k, 0), nt, preferred_element_type=F32
        ).astype(BF)
        up_out[0, :, cols] = lax.dot_general(
            pick, stacked(gu, k, 1), nt, preferred_element_type=F32
        ).astype(BF)
        sd_out[:, cols] = lax.dot_general(
            same, stacked(sh, k, 2), nt, preferred_element_type=F32
        ).astype(BF)
        sg_out[cols, :] = stacked(sh, k, 0)
        su_out[cols, :] = stacked(sh, k, 1)
    for k in range(ys // 2):
        left = dd[pl.ds(2 * k * share, share)].reshape(wide_share, LANES)
        right = dd[pl.ds((2 * k + 1) * share, share)].reshape(wide_share, LANES)
        left = lax.dot_general(left, pick, nt, preferred_element_type=F32)
        right = lax.dot_general(right, pick, nt, preferred_element_type=F32)
        down_out[0, :, pl.ds(k * LANES, LANES)] = jnp.concatenate([left, right], axis=1).astype(BF)

    await_bytes(part_in.at[pl.ds(0, ys - 1)], recv.at[7])
    shared_sum = sum(part_in[k].astype(F32) for k in range(ys))
    by_slot = jnp.where(first, weight[0:1, :].reshape(1, 1, LANES), 0.0) + jnp.where(
        second, weight[1:2, :].reshape(1, 1, LANES), 0.0
    )
    by_slot = jnp.where(position == slot_f, by_slot.reshape(experts * slab, LANES), 0.0)
    high = by_slot.astype(BF)
    low = (by_slot - high.astype(F32)).astype(BF)
    none = jnp.zeros_like(high)
    tn = (((0,), (0,)), ((), ()))
    await_bytes(back_in.at[pl.ds(0, others)], recv.at[11])
    arrived = back_in[...].reshape(experts * slab, LANES)
    for k in range(4):
        here = block_2d == k
        routed = lax.dot_general(
            jnp.where(here, high, none), arrived, tn, preferred_element_type=F32
        ) + lax.dot_general(jnp.where(here, low, none), arrived, tn, preferred_element_type=F32)
        lanes = slice(k * LANES, (k + 1) * LANES)
        mixed[:, lanes] = (shared_sum[:, lanes] + routed).astype(BF)

    await_bytes(sh.at[pl.ds(0, 3), c], send.at[0])
    await_bytes(tok_src.at[pl.ds(0, others)], send.at[1])
    await_bytes(sh.at[pl.ds(0, 4 * (quarter - 1)), c], send.at[2])
    await_bytes(gu_src.at[pl.ds(0, others)], send.at[3])
    await_bytes(down_src.at[pl.ds(0, others)], send.at[4])
    await_bytes(sh.at[pl.ds(0, (xs - 1) * zs), c], send.at[5])
    await_bytes(sh.at[:, c], send.at[6])
    await_bytes(part_src.at[pl.ds(0, ys - 1)], send.at[7])
    await_bytes(gu.at[:, c], send.at[8])
    await_bytes(down_in.at[pl.ds(0, (ys - 1) * share)], send.at[9])
    await_bytes(dd.at[:, c], send.at[10])
    await_bytes(back_src.at[pl.ds(0, others)], send.at[11])
    ring_drain(own_tok, tok_sem)
    ring_drain(rows, row_sem)
    ring_drain(hid, hid_sem)


def on_device(zs, xs, ys, tokens, routes, route_weight, norm_gain, e_gate, e_up, e_down, s_gate, s_up, s_down):
    experts, d_rows, _ = e_gate.shape
    tok_count, width = tokens.shape
    slab = 4 * CAP
    turn = turn_matrix()
    gain = jnp.broadcast_to(norm_gain[:, None], (d_rows, LANES))
    all_rows = experts * CAP
    model = experts * 2 * d_rows
    vmem = pl.BlockSpec(memory_space=pltpu.VMEM)
    outs = pl.pallas_call(
        functools.partial(kernel, zs, xs, ys),
        out_shape=(
            jax.ShapeDtypeStruct((tok_count, width), BF),
            jax.ShapeDtypeStruct((1, 64, model), BF),
            jax.ShapeDtypeStruct((1, 64, model), BF),
            jax.ShapeDtypeStruct((1, width, 2 * LANES), BF),
            jax.ShapeDtypeStruct((model, LANES), BF),
            jax.ShapeDtypeStruct((model, LANES), BF),
            jax.ShapeDtypeStruct((LANES, model), BF),
        ),
        in_specs=[vmem] * 12,
        out_specs=(vmem,) * 7,
        scratch_shapes=[
            pltpu.VMEM((experts, slab, LANES), BF),
            pltpu.VMEM((experts, 2, d_rows, LANES), BF),
            pltpu.VMEM((experts, d_rows, LANES), BF),
            pltpu.VMEM((experts, slab, LANES), BF),
            pltpu.VMEM((experts, 2, 2, d_rows, LANES), BF),
            pltpu.VMEM((experts, d_rows, LANES), BF),
            pltpu.VMEM((experts, 2, d_rows, LANES), BF),
            pltpu.VMEM((experts, 2, 3, d_rows, LANES), BF),
            pltpu.VMEM((ys, tok_count, width), BF),
            pltpu.VMEM((ys, all_rows, width), BF),
            pltpu.VMEM((ys, all_rows, width), BF),
            pltpu.VMEM((ys, all_rows, LANES), BF),
            pltpu.VMEM((ys, tok_count, width), BF),
            pltpu.VMEM((ys, tok_count, width), BF),
            pltpu.VMEM((experts, slab, LANES), BF),
            pltpu.VMEM((experts, slab, LANES), BF),
            pltpu.SemaphoreType.DMA((12,)),
            pltpu.SemaphoreType.DMA((12,)),
            pltpu.SemaphoreType.DMA((8,)),
            pltpu.SemaphoreType.DMA((8,)),
            pltpu.SemaphoreType.DMA((8,)),
        ],
        compiler_params=pltpu.CompilerParams(
            collective_id=0, has_side_effects=True, vmem_limit_bytes=44 * 1024 * 1024
        ),
    )(
        tokens, routes.T, route_weight.T, gain, e_gate, e_up, e_down, s_gate, s_up, s_down.T,
        jnp.asarray(turn, BF), jnp.asarray(turn.T, BF),
    )
    mixed, gate_t, up_t, down_new, sg, su, sd = outs
    return (
        mixed, gate_t.transpose(0, 2, 1), up_t.transpose(0, 2, 1), down_new, sg, su, sd,
    )


def solution(mesh):
    tp = mesh.shape["tp"]
    devices = mesh.devices.reshape(16, 4, 2, tp)
    split = Mesh(devices, ("z", "x", "c", "y"))
    zs, xs, _, ys = devices.shape
    placed = (
        P(FS, "y"),
        P(FS, None),
        P(FS, None),
        P(FS),
        P(None, FS, "y"),
        P(None, FS, "y"),
        P(None, FS, "y"),
        P(FS, "y"),
        P(FS, "y"),
        P("y", FS),
    )
    return jax.shard_map(
        functools.partial(on_device, zs, xs, ys),
        mesh=split,
        in_specs=placed,
        out_specs=(
            P(FS, "y"),
            P(FS, None, "y"),
            P(FS, None, "y"),
            P(FS, "y", None),
            P(None, "y"),
            P(None, "y"),
            P("y", None),
        ),
        check_vma=False,
    )
```

```python
import functools

import jax
import jax.numpy as jnp
import numpy as np
from jax import lax
from jax.experimental import pallas as pl
from jax.experimental.pallas import tpu as pltpu
from jax.sharding import Mesh
from jax.sharding import PartitionSpec as P

FS = ("z", "x", "c")
EPS = 1e-06
MESH = pl.DeviceIdType.MESH
BF = jnp.bfloat16
F32 = jnp.float32
CAP = 6
LANES = 128


def turn_matrix():
    turn = np.zeros((8 * 4 * CAP, 8 * 4 * CAP), np.float32)
    for block in range(4):
        for source in range(8):
            for slot in range(CAP):
                turn[block * 8 * CAP + source * CAP + slot, source * 4 * CAP + block * CAP + slot] = 1
    return turn


def peer_at(step, z, x, zs, xs):
    pair = step // xs
    dz = pair // 2 + 1 - (zs // 2) * (pair % 2)
    dx = (step % xs + 1) % xs
    return lax.rem(z + dz + zs, zs), lax.rem(x + dx, xs)


def await_bytes(ref, sem):
    pltpu.make_async_copy(ref, ref, sem).wait()


def kernel(
    zs, xs, ys,
    tok_hbm, route_hbm, weight_hbm, gain_hbm, gate_hbm, up_hbm, down_hbm, s_gate_hbm, s_up_hbm,
    s_down_hbm, turn_hbm, turn_back_hbm,
    mixed_hbm, gate_hbm_out, up_hbm_out, down_hbm_out, sg_hbm_out, su_hbm_out, sd_hbm_out,
    mixed, gate_out, up_out, down_out, sg_out, su_out, sd_out,
    tok_src, gu_src, down_src, tok_in, gu, dd, sh, own_tok, rows, normed, hid,
    part_src, part_in, result, back_src, back_in,
    tok, route, weight, gain, gate, up, down, s_gate, s_up, s_down, turn, turn_back,
    send, recv, row_sem, load_sem, store_sem,
):
    z, x, c, y = (lax.axis_index(a) for a in ("z", "x", "c", "y"))
    me = z * xs + x
    others = zs * xs - 1
    above, below = lax.rem(y + 1, ys), lax.rem(y + ys - 1, ys)
    far = lax.rem(y + 2, ys)

    loads = {}
    for number, (name, src, dst) in enumerate((
        ("route", route_hbm, route), ("tok", tok_hbm, tok), ("gain", gain_hbm, gain),
        ("gate", gate_hbm, gate), ("up", up_hbm, up), ("down", down_hbm, down),
        ("s_gate", s_gate_hbm, s_gate), ("s_up", s_up_hbm, s_up), ("s_down", s_down_hbm, s_down),
        ("weight", weight_hbm, weight), ("turn", turn_hbm, turn),
        ("turn_back", turn_back_hbm, turn_back),
    )):
        loads[name] = pltpu.make_async_copy(src, dst, load_sem.at[number])
        loads[name].start()

    barrier = pltpu.get_barrier_semaphore()

    def greet(step, carry):
        pz, px = peer_at(step, z, x, zs, xs)
        pl.semaphore_signal(barrier, inc=1, device_id={"z": pz, "x": px}, device_id_type=MESH)
        return carry

    lax.fori_loop(0, others, greet, 0)
    for k in range(1, ys):
        pl.semaphore_signal(
            barrier, inc=1, device_id={"y": lax.rem(y + k, ys)}, device_id_type=MESH
        )
    pl.semaphore_signal(barrier, inc=1, device_id={"c": 1 - c}, device_id_type=MESH)
    part_z = zs // ys
    owner = z // part_z

    def greet_sources(step, carry):
        pz = y * part_z + step // xs
        for k in range(1, ys):
            pl.semaphore_signal(
                barrier, inc=1,
                device_id={"z": pz, "x": lax.rem(step, xs), "y": lax.rem(y + k, ys)},
                device_id_type=MESH,
            )
        return carry

    lax.fori_loop(0, part_z * xs, greet_sources, 0)

    loads["route"].wait()
    loads["tok"].wait()
    experts = zs * xs
    slab = 4 * CAP
    shape = (experts, slab, LANES)
    expert_id = lax.broadcasted_iota(jnp.int32, shape, 0)
    place = lax.broadcasted_iota(jnp.int32, shape, 1)
    block = (
        (place >= CAP).astype(jnp.int32)
        + (place >= 2 * CAP).astype(jnp.int32)
        + (place >= 3 * CAP).astype(jnp.int32)
    )
    slot = place - CAP * block
    first = route[0:1, :].reshape(1, 1, LANES) == expert_id
    second = route[1:2, :].reshape(1, 1, LANES) == expert_id
    named = (first | second).astype(F32).reshape(experts * slab, LANES)
    before = (
        lax.broadcasted_iota(jnp.int32, (LANES, LANES), 0)
        < lax.broadcasted_iota(jnp.int32, (LANES, LANES), 1)
    ).astype(BF)
    position = jnp.dot(named.astype(BF), before, preferred_element_type=F32)
    slot_f = slot.astype(F32).reshape(experts * slab, LANES)
    picked = jnp.where(position == slot_f, named, 0.0)
    chosen = jnp.dot(picked.astype(BF), tok[...], preferred_element_type=F32)
    block_2d = block.reshape(experts * slab, LANES)
    packed = chosen[:, 0:LANES]
    for k in range(1, 4):
        packed = jnp.where(block_2d == k, chosen[:, k * LANES : (k + 1) * LANES], packed)
    tok_src[...] = packed.astype(BF).reshape(shape)
    loads["gain"].wait()
    rows_gain = jnp.sum(
        jnp.where(
            lax.broadcasted_iota(jnp.int32, (16, 16), 0)
            == lax.broadcasted_iota(jnp.int32, (16, 16), 1),
            jnp.broadcast_to(gain[...].reshape(1, 16), (16, 16)),
            0.0,
        ),
        axis=1,
        keepdims=True,
    )
    scale = rows_gain[None]
    for name in ("s_gate", "s_up", "s_down", "gate", "up", "down"):
        loads[name].wait()
    gu_src[:, 0] = (gate[...] * scale).astype(BF)
    gu_src[:, 1] = (up[...] * scale).astype(BF)
    down_src[...] = down[...].astype(BF)
    sh[z, x, c, 0] = (s_gate[...] * rows_gain).astype(BF)
    sh[z, x, c, 1] = (s_up[...] * rows_gain).astype(BF)
    sh[z, x, c, 2] = s_down[...].astype(BF)
    own_tok[y] = tok[...]
    tok_in[me] = tok_src[me]
    gu[me, c] = gu_src[me]

    for name in ("weight", "turn", "turn_back"):
        loads[name].wait()
    pl.semaphore_wait(barrier, others + ys + jnp.where(owner == y, 0, experts))

    def remote(src, dst, send_sem, recv_sem, to):
        return pltpu.make_async_remote_copy(
            src_ref=src, dst_ref=dst, send_sem=send_sem, recv_sem=recv_sem,
            device_id=to, device_id_type=MESH,
        )

    def ring_start(buf, sems):
        remote(buf.at[y], buf.at[y], sems.at[0], sems.at[4], {"y": above}).start()
        remote(buf.at[y], buf.at[y], sems.at[1], sems.at[5], {"y": below}).start()

    def ring_forward(buf, sems):
        half = buf.shape[1] // 2
        await_bytes(buf.at[below], sems.at[4])
        low = buf.at[below, pl.ds(0, half)]
        remote(low, low, sems.at[2], sems.at[6], {"y": above}).start()
        await_bytes(buf.at[above], sems.at[5])
        high = buf.at[above, pl.ds(half, half)]
        remote(high, high, sems.at[3], sems.at[7], {"y": below}).start()

    def ring_finish(buf, sems):
        half = buf.shape[1] // 2
        await_bytes(buf.at[far, pl.ds(0, half)], sems.at[6])
        await_bytes(buf.at[far, pl.ds(half, half)], sems.at[7])

    def ring_drain(buf, sems):
        half = buf.shape[1] // 2
        await_bytes(buf.at[y], sems.at[0])
        await_bytes(buf.at[y], sems.at[1])
        await_bytes(buf.at[y, pl.ds(0, half)], sems.at[2])
        await_bytes(buf.at[y, pl.ds(0, half)], sems.at[3])

    def spread_along_y(buf, number):
        for k in range(1, ys):
            to = lax.rem(y + k, ys)
            remote(buf.at[y], buf.at[y], send.at[number], recv.at[number], {"y": to}).start()

    def to_columns(src_at, dst_at, number, to_y=None):
        def one(step, carry):
            pz, px = peer_at(step, z, x, zs, xs)
            to = {"z": pz, "x": px}
            if to_y is not None:
                to["y"] = to_y
            remote(src_at(pz * xs + px), dst_at, send.at[number], recv.at[number], to).start()
            return carry

        lax.fori_loop(0, others, one, 0)

    quarter = zs // 4
    for k in range(1, 4):
        pz = lax.rem(z + k * quarter, zs)
        own = sh.at[z, x, c]
        remote(own, own, send.at[0], recv.at[0], {"z": pz}).start()
    spread_along_y(own_tok, 5)
    to_columns(lambda e: tok_src.at[e], tok_in.at[me], 1)
    to_columns(lambda e: gu_src.at[e], gu.at[me, c], 3)
    share = experts // ys
    down_at = dd.at[y * share + lax.rem(z, part_z) * xs + x, c]

    @pl.when(owner == y)
    def _():
        pltpu.make_async_copy(down_src.at[me], down_at, recv.at[4]).start()

    @pl.when(owner != y)
    def _():
        remote(down_src.at[me], down_at, send.at[9], recv.at[4], {"y": owner}).start()

    to_columns(lambda e: down_src.at[e], down_at, 4, owner)
    await_bytes(sh.at[pl.ds(0, 3), x, c], recv.at[0])
    for k in range(1, quarter):
        pz = lax.rem(z - z % quarter + (z + k) % quarter, zs)
        for q in range(4):
            piece = sh.at[z % quarter + q * quarter, x, c]
            remote(piece, piece, send.at[2], recv.at[2], {"z": pz}).start()

    await_bytes(tok_in.at[pl.ds(0, others)], recv.at[1])
    group = 8 * CAP
    for g in range(experts // 8):
        lines = tok_in[pl.ds(8 * g, 8)].reshape(8 * slab, LANES)
        turned = jnp.dot(turn[...], lines, preferred_element_type=F32).astype(BF)
        for k in range(4):
            rows[y, pl.ds(g * group, group), pl.ds(k * LANES, LANES)] = turned[
                k * group : (k + 1) * group
            ]
    ring_start(rows, row_sem)

    await_bytes(own_tok.at[pl.ds(0, ys - 1)], recv.at[5])
    wide = [own_tok[k].astype(F32) for k in range(ys)]
    total = sum(jnp.sum(w * w, axis=1, keepdims=True) for w in wide)
    factor = lax.rsqrt(total * (1.0 / (ys * tok.shape[1])) + EPS)
    own_normed = [(w * factor).astype(BF) for w in wide]

    ring_forward(rows, row_sem)

    ring_finish(rows, row_sem)
    row_total = jnp.zeros((rows.shape[1], 1), F32)
    for k in range(ys):
        part = rows[k].astype(F32)
        row_total = row_total + jnp.sum(part * part, axis=1, keepdims=True)
    row_factor = lax.rsqrt(row_total * (1.0 / (ys * tok.shape[1])) + EPS)
    for k in range(ys):
        normed[k] = (rows[k].astype(F32) * row_factor).astype(BF)

    nt = (((1,), (1,)), ((), ()))

    def shared_rows(k, number):
        return sh[pl.ds(k * part_z, part_z), :, :, number].reshape(share * 2 * 16, LANES)

    def stacked(ref, k, number):
        return ref[pl.ds(k * share, share), :, number].reshape(share * 2 * 16, LANES)

    await_bytes(gu.at[pl.ds(0, others), c], recv.at[3])
    remote(gu.at[:, c], gu.at[:, c], send.at[8], recv.at[8], {"c": 1 - c}).start()
    await_bytes(gu.at[:, c], recv.at[8])
    act = sum(
        jnp.dot(normed[k], stacked(gu, k, 0), preferred_element_type=F32) for k in range(ys)
    )
    lin = sum(
        jnp.dot(normed[k], stacked(gu, k, 1), preferred_element_type=F32) for k in range(ys)
    )
    hid[y] = (act / (1.0 + jnp.exp(-act)) * lin).astype(BF)
    spread_along_y(hid, 12)

    half_rows = lax.broadcasted_iota(jnp.int32, (64, LANES), 0) + 64 * c
    pick = (half_rows == lax.broadcasted_iota(jnp.int32, (64, LANES), 1)).astype(BF)
    wide_share = share * 2 * 16
    for k in range(ys):
        cols = pl.ds(k * wide_share, wide_share)
        gate_out[0, :, cols] = lax.dot_general(
            pick, stacked(gu, k, 0), nt, preferred_element_type=F32
        ).astype(BF)
        up_out[0, :, cols] = lax.dot_general(
            pick, stacked(gu, k, 1), nt, preferred_element_type=F32
        ).astype(BF)
    stores = [
        pltpu.make_async_copy(src, dst, store_sem.at[number])
        for number, (src, dst) in enumerate((
            (gate_out, gate_hbm_out), (up_out, up_hbm_out), (down_out, down_hbm_out),
            (sg_out, sg_hbm_out), (su_out, su_hbm_out), (sd_out, sd_hbm_out),
            (mixed, mixed_hbm),
        ))
    ]
    for store in stores[:2]:
        store.start()

    await_bytes(dd.at[:, c], recv.at[4])
    remote(dd.at[:, c], dd.at[:, c], send.at[10], recv.at[10], {"c": 1 - c}).start()
    await_bytes(hid.at[pl.ds(0, ys - 1)], recv.at[12])
    await_bytes(dd.at[:, c], recv.at[10])
    result[...] = sum(
        lax.dot_general(
            hid[k], dd[pl.ds(k * share, share)].reshape(wide_share, LANES), nt,
            preferred_element_type=F32,
        )
        for k in range(ys)
    ).astype(BF)

    await_bytes(sh.at[pl.ds(0, 4 * (quarter - 1)), x, c], recv.at[2])
    for k in range(1, xs):
        line = sh.at[:, x, c]
        remote(line, line, send.at[13], recv.at[13], {"x": lax.rem(x + k, xs)}).start()

    groups = experts // 8

    def send_back(g, count):
        def one(step, carry):
            pz = lax.rem(2 * g + (step // xs) + (z + 1) % 2, 2) + 2 * g
            px = lax.rem(x + 1 + lax.rem(step, xs), xs)
            remote(
                back_src.at[pz * xs + px], back_in.at[me], send.at[11], recv.at[11],
                {"z": pz, "x": px},
            ).start()
            return carry

        lax.fori_loop(0, count, one, 0)

    previous = None
    for offset in (4, 3, 5, 2, 6, 1, 7, 0):
        g = lax.rem(z // 2 + offset, groups)
        part = result[pl.ds(pl.multiple_of(g * group, 16), group), :]
        lines = jnp.concatenate([part[:, k * LANES : (k + 1) * LANES] for k in range(4)], axis=0)
        turned = jnp.dot(turn_back[...], lines, preferred_element_type=F32).astype(BF)
        back_src[pl.ds(8 * g, 8)] = turned.reshape(8, slab, LANES)
        if previous is not None:
            send_back(previous, 8)
        previous = g
    back_in[me] = back_src[me]
    send_back(previous, 7)

    for k in range(ys // 2):
        left = dd[pl.ds(2 * k * share, share)].reshape(wide_share, LANES)
        right = dd[pl.ds((2 * k + 1) * share, share)].reshape(wide_share, LANES)
        left = lax.dot_general(left, pick, nt, preferred_element_type=F32)
        right = lax.dot_general(right, pick, nt, preferred_element_type=F32)
        down_out[0, :, pl.ds(k * LANES, LANES)] = jnp.concatenate([left, right], axis=1).astype(BF)
    stores[2].start()
    await_bytes(sh.at[:, pl.ds(0, xs - 1), c], recv.at[13])
    half = sh.at[:, :, c]
    remote(half, half, send.at[6], recv.at[6], {"c": 1 - c}).start()
    await_bytes(half, recv.at[6])
    act = sum(
        jnp.dot(own_normed[k], shared_rows(k, 0), preferred_element_type=F32) for k in range(ys)
    )
    lin = sum(
        jnp.dot(own_normed[k], shared_rows(k, 1), preferred_element_type=F32) for k in range(ys)
    )
    shared_hidden = (act / (1.0 + jnp.exp(-act)) * lin).astype(BF)
    for k in range(ys):
        part_src[k] = lax.dot_general(
            shared_hidden, shared_rows(k, 2), nt, preferred_element_type=F32
        ).astype(BF)
    part_in[y] = part_src[y]
    for k in range(1, ys):
        to = lax.rem(y + k, ys)
        remote(part_src.at[to], part_in.at[y], send.at[7], recv.at[7], {"y": to}).start()

    same = (
        lax.broadcasted_iota(jnp.int32, (LANES, LANES), 0)
        == lax.broadcasted_iota(jnp.int32, (LANES, LANES), 1)
    ).astype(BF)
    for k in range(ys):
        cols = pl.ds(k * wide_share, wide_share)
        sd_out[:, cols] = lax.dot_general(
            same, shared_rows(k, 2), nt, preferred_element_type=F32
        ).astype(BF)
        sg_out[cols, :] = shared_rows(k, 0)
        su_out[cols, :] = shared_rows(k, 1)
    for store in stores[3:-1]:
        store.start()

    await_bytes(part_in.at[pl.ds(0, ys - 1)], recv.at[7])
    shared_sum = sum(part_in[k].astype(F32) for k in range(ys))
    by_slot = jnp.where(first, weight[0:1, :].reshape(1, 1, LANES), 0.0) + jnp.where(
        second, weight[1:2, :].reshape(1, 1, LANES), 0.0
    )
    by_slot = jnp.where(position == slot_f, by_slot.reshape(experts * slab, LANES), 0.0)
    high = by_slot.astype(BF)
    low = (by_slot - high.astype(F32)).astype(BF)
    none = jnp.zeros_like(high)
    tn = (((0,), (0,)), ((), ()))
    await_bytes(back_in.at[pl.ds(0, others)], recv.at[11])
    arrived = back_in[...].reshape(experts * slab, LANES)
    for k in range(4):
        here = block_2d == k
        routed = lax.dot_general(
            jnp.where(here, high, none), arrived, tn, preferred_element_type=F32
        ) + lax.dot_general(jnp.where(here, low, none), arrived, tn, preferred_element_type=F32)
        lanes = slice(k * LANES, (k + 1) * LANES)
        mixed[:, lanes] = (shared_sum[:, lanes] + routed).astype(BF)

    stores[-1].start()

    await_bytes(sh.at[pl.ds(0, 3), x, c], send.at[0])
    await_bytes(tok_src.at[pl.ds(0, others)], send.at[1])
    await_bytes(sh.at[pl.ds(0, 4 * (quarter - 1)), x, c], send.at[2])
    await_bytes(gu_src.at[pl.ds(0, others)], send.at[3])
    await_bytes(down_src.at[pl.ds(0, others)], send.at[4])
    await_bytes(own_tok.at[pl.ds(0, ys - 1)], send.at[5])
    await_bytes(hid.at[pl.ds(0, ys - 1)], send.at[12])
    await_bytes(sh.at[:, pl.ds(0, xs - 1), c], send.at[13])
    await_bytes(sh.at[:, :, c], send.at[6])
    await_bytes(part_src.at[pl.ds(0, ys - 1)], send.at[7])
    await_bytes(gu.at[:, c], send.at[8])

    @pl.when(owner != y)
    def _():
        await_bytes(down_src.at[me], send.at[9])

    await_bytes(dd.at[:, c], send.at[10])
    await_bytes(back_src.at[pl.ds(0, others)], send.at[11])
    ring_drain(rows, row_sem)
    for store in stores:
        store.wait()


def write_out(*refs):
    sources, targets, held, sems = refs[:7], refs[7:14], refs[14:21], refs[21]
    into = [pltpu.make_async_copy(sources[k], held[k], sems.at[k]) for k in range(7)]
    out = [pltpu.make_async_copy(held[k], targets[k], sems.at[7 + k]) for k in range(7)]
    for copy in into:
        copy.start()
    for k in range(7):
        into[k].wait()
        out[k].start()
    for copy in out:
        copy.wait()


def on_device(zs, xs, ys, tokens, routes, route_weight, norm_gain, e_gate, e_up, e_down, s_gate, s_up, s_down):
    experts, d_rows, _ = e_gate.shape
    tok_count, width = tokens.shape
    slab = 4 * CAP
    turn = turn_matrix()
    all_rows = experts * CAP
    model = experts * 2 * d_rows
    hbm = pl.BlockSpec(memory_space=pltpu.HBM)
    made = (
        ((tok_count, width), BF),
        ((1, 64, model), BF),
        ((1, 64, model), BF),
        ((1, width, 2 * LANES), BF),
        ((model, LANES), BF),
        ((model, LANES), BF),
        ((LANES, model), BF),
    )
    outs = pl.pallas_call(
        functools.partial(kernel, zs, xs, ys),
        out_shape=tuple(jax.ShapeDtypeStruct(*m) for m in made),
        in_specs=[hbm] * 12,
        out_specs=(hbm,) * 7,
        scratch_shapes=[pltpu.VMEM(*m) for m in made]
        + [
            pltpu.VMEM((experts, slab, LANES), BF),
            pltpu.VMEM((experts, 2, d_rows, LANES), BF),
            pltpu.VMEM((experts, d_rows, LANES), BF),
            pltpu.VMEM((experts, slab, LANES), BF),
            pltpu.VMEM((experts, 2, 2, d_rows, LANES), BF),
            pltpu.VMEM((experts, 2, d_rows, LANES), BF),
            pltpu.VMEM((zs, xs, 2, 3, d_rows, LANES), BF),
            pltpu.VMEM((ys, tok_count, width), BF),
            pltpu.VMEM((ys, all_rows, width), BF),
            pltpu.VMEM((ys, all_rows, width), BF),
            pltpu.VMEM((ys, all_rows, LANES), BF),
            pltpu.VMEM((ys, tok_count, width), BF),
            pltpu.VMEM((ys, tok_count, width), BF),
            pltpu.VMEM((all_rows, width), BF),
            pltpu.VMEM((experts, slab, LANES), BF),
            pltpu.VMEM((experts, slab, LANES), BF),
            pltpu.VMEM((tok_count, width), BF),
            pltpu.VMEM((2, LANES), jnp.int32),
            pltpu.VMEM((2, LANES), F32),
            pltpu.VMEM((d_rows,), F32),
            pltpu.VMEM((experts, d_rows, LANES), F32),
            pltpu.VMEM((experts, d_rows, LANES), F32),
            pltpu.VMEM((experts, d_rows, LANES), F32),
            pltpu.VMEM((d_rows, LANES), F32),
            pltpu.VMEM((d_rows, LANES), F32),
            pltpu.VMEM((d_rows, LANES), F32),
            pltpu.VMEM(turn.shape, BF),
            pltpu.VMEM(turn.shape, BF),
            pltpu.SemaphoreType.DMA((14,)),
            pltpu.SemaphoreType.DMA((14,)),
            pltpu.SemaphoreType.DMA((8,)),
            pltpu.SemaphoreType.DMA((12,)),
            pltpu.SemaphoreType.DMA((7,)),
        ],
        compiler_params=pltpu.CompilerParams(
            collective_id=0, has_side_effects=True, vmem_limit_bytes=61000 * 1024
        ),
    )(
        tokens, routes.T, route_weight.T, norm_gain, e_gate, e_up, e_down, s_gate, s_up, s_down.T,
        jnp.asarray(turn, BF), jnp.asarray(turn.T, BF),
    )
    mixed, gate_t, up_t, down_new, sg, su, sd = pl.pallas_call(
        write_out,
        out_shape=tuple(jax.ShapeDtypeStruct(o.shape, o.dtype) for o in outs),
        in_specs=[hbm] * 7,
        out_specs=(hbm,) * 7,
        scratch_shapes=[pltpu.VMEM(*m) for m in made] + [pltpu.SemaphoreType.DMA((14,))],
        compiler_params=pltpu.CompilerParams(vmem_limit_bytes=61000 * 1024),
    )(*outs)
    return (
        mixed, gate_t.transpose(0, 2, 1), up_t.transpose(0, 2, 1), down_new, sg, su, sd,
    )


def solution(mesh):
    tp = mesh.shape["tp"]
    devices = mesh.devices.reshape(16, 4, 2, tp)
    split = Mesh(devices, ("z", "x", "c", "y"))
    zs, xs, _, ys = devices.shape
    placed = (
        P(FS, "y"),
        P(FS, None),
        P(FS, None),
        P(FS),
        P(None, FS, "y"),
        P(None, FS, "y"),
        P(None, FS, "y"),
        P(FS, "y"),
        P(FS, "y"),
        P("y", FS),
    )
    return jax.shard_map(
        functools.partial(on_device, zs, xs, ys),
        mesh=split,
        in_specs=placed,
        out_specs=(
            P(FS, "y"),
            P(FS, None, "y"),
            P(FS, None, "y"),
            P(FS, "y", None),
            P(None, "y"),
            P(None, "y"),
            P("y", None),
        ),
        check_vma=False,
    )
```

```python
import functools

import jax
import jax.numpy as jnp
import numpy as np
from jax import lax
from jax.experimental import pallas as pl
from jax.experimental.pallas import tpu as pltpu
from jax.sharding import Mesh
from jax.sharding import PartitionSpec as P

FS = ("z", "x", "c")
EPS = 1e-06
MESH = pl.DeviceIdType.MESH
BF = jnp.bfloat16
F32 = jnp.float32
CAP = 6
LANES = 128


def turn_matrix():
    turn = np.zeros((8 * 4 * CAP, 8 * 4 * CAP), np.float32)
    for block in range(4):
        for source in range(8):
            for slot in range(CAP):
                turn[block * 8 * CAP + source * CAP + slot, source * 4 * CAP + block * CAP + slot] = 1
    return turn


def peer_at(step, z, x, zs, xs):
    pair = step // xs
    dz = pair // 2 + 1 - (zs // 2) * (pair % 2)
    dx = (step % xs + 1) % xs
    return lax.rem(z + dz + zs, zs), lax.rem(x + dx, xs)


def await_bytes(ref, sem):
    pltpu.make_async_copy(ref, ref, sem).wait()


def kernel(
    zs, xs, ys,
    tok_hbm, route_hbm, weight_hbm, gain_hbm, gate_hbm, up_hbm, down_hbm, s_gate_hbm, s_up_hbm,
    s_down_hbm, turn_hbm, turn_back_hbm,
    mixed_hbm, gate_hbm_out, up_hbm_out, down_hbm_out, sg_hbm_out, su_hbm_out, sd_hbm_out,
    mixed, gate_out, up_out, down_out, sg_out, su_out, sd_out,
    tok_src, gu_src, down_src, tok_in, gu, dd, sh, own_tok, rows, normed, hid,
    part_src, part_in, result, back_src, back_in,
    tok, route, weight, gain, gate, up, down, s_gate, s_up, s_down, turn, turn_back,
    send, recv, row_sem, load_sem, store_sem,
):
    z, x, c, y = (lax.axis_index(a) for a in ("z", "x", "c", "y"))
    me = z * xs + x
    fourth = zs // 4
    q, r = z // fourth, z % fourth
    others = zs * xs - 1
    above, below = lax.rem(y + 1, ys), lax.rem(y + ys - 1, ys)
    far = lax.rem(y + 2, ys)

    barrier = pltpu.get_barrier_semaphore()

    def greet(step, carry):
        pair = step // xs
        dz = (zs // 2 - (pair + 1) // 2) * (2 * (pair % 2) - 1)
        pz, px = lax.rem(z + dz + zs, zs), lax.rem(x + 1 + step % xs, xs)
        pl.semaphore_signal(barrier, inc=1, device_id={"z": pz, "x": px}, device_id_type=MESH)
        return carry

    lax.fori_loop(0, others, greet, 0)
    for k in range(1, ys):
        pl.semaphore_signal(
            barrier, inc=1, device_id={"y": lax.rem(y + k, ys)}, device_id_type=MESH
        )
    pl.semaphore_signal(barrier, inc=1, device_id={"c": 1 - c}, device_id_type=MESH)
    part_z = zs // ys
    owner = z // part_z

    def greet_sources(step, carry):
        pz = y * part_z + step // xs
        for k in range(1, ys):
            pl.semaphore_signal(
                barrier, inc=1,
                device_id={"z": pz, "x": lax.rem(step, xs), "y": lax.rem(y + k, ys)},
                device_id_type=MESH,
            )
        return carry

    lax.fori_loop(0, part_z * xs, greet_sources, 0)

    loads = {}
    for number, (name, src, dst) in enumerate((
        ("route", route_hbm, route), ("tok", tok_hbm, tok), ("gain", gain_hbm, gain),
        ("gate", gate_hbm, gate), ("up", up_hbm, up), ("down", down_hbm, down),
        ("s_gate", s_gate_hbm, s_gate), ("s_up", s_up_hbm, s_up), ("s_down", s_down_hbm, s_down),
        ("weight", weight_hbm, weight), ("turn", turn_hbm, turn),
        ("turn_back", turn_back_hbm, turn_back),
    )):
        loads[name] = pltpu.make_async_copy(src, dst, load_sem.at[number])
        loads[name].start()

    loads["route"].wait()
    loads["tok"].wait()
    experts = zs * xs
    slab = 4 * CAP
    shape = (experts, slab, LANES)
    expert_id = lax.broadcasted_iota(jnp.int32, shape, 0)
    place = lax.broadcasted_iota(jnp.int32, shape, 1)
    block = (
        (place >= CAP).astype(jnp.int32)
        + (place >= 2 * CAP).astype(jnp.int32)
        + (place >= 3 * CAP).astype(jnp.int32)
    )
    slot = place - CAP * block
    first = route[0:1, :].reshape(1, 1, LANES) == expert_id
    second = route[1:2, :].reshape(1, 1, LANES) == expert_id
    named = (first | second).astype(F32).reshape(experts * slab, LANES)
    before = (
        lax.broadcasted_iota(jnp.int32, (LANES, LANES), 0)
        < lax.broadcasted_iota(jnp.int32, (LANES, LANES), 1)
    ).astype(BF)
    position = jnp.dot(named.astype(BF), before, preferred_element_type=F32)
    slot_f = slot.astype(F32).reshape(experts * slab, LANES)
    picked = jnp.where(position == slot_f, named, 0.0)
    chosen = jnp.dot(picked.astype(BF), tok[...], preferred_element_type=F32)
    block_2d = block.reshape(experts * slab, LANES)
    packed = chosen[:, 0:LANES]
    for k in range(1, 4):
        packed = jnp.where(block_2d == k, chosen[:, k * LANES : (k + 1) * LANES], packed)
    tok_src[...] = packed.astype(BF).reshape(shape)
    loads["gain"].wait()
    rows_gain = jnp.sum(
        jnp.where(
            lax.broadcasted_iota(jnp.int32, (16, 16), 0)
            == lax.broadcasted_iota(jnp.int32, (16, 16), 1),
            jnp.broadcast_to(gain[...].reshape(1, 16), (16, 16)),
            0.0,
        ),
        axis=1,
        keepdims=True,
    )
    scale = rows_gain[None]
    for name in ("s_gate", "s_up", "s_down", "gate", "up", "down"):
        loads[name].wait()
    gu_src[:, 0] = (gate[...] * scale).astype(BF)
    gu_src[:, 1] = (up[...] * scale).astype(BF)
    down_src[...] = down[...].astype(BF)
    sh[q, r, x, c, 0] = (s_gate[...] * rows_gain).astype(BF)
    sh[q, r, x, c, 1] = (s_up[...] * rows_gain).astype(BF)
    sh[q, r, x, c, 2] = s_down[...].astype(BF)
    own_tok[y] = tok[...]
    tok_in[me] = tok_src[me]
    gu[me, c] = gu_src[me]

    for name in ("weight", "turn", "turn_back"):
        loads[name].wait()
    pl.semaphore_wait(barrier, others + ys + jnp.where(owner == y, 0, experts))

    def remote(src, dst, send_sem, recv_sem, to):
        return pltpu.make_async_remote_copy(
            src_ref=src, dst_ref=dst, send_sem=send_sem, recv_sem=recv_sem,
            device_id=to, device_id_type=MESH,
        )

    def ring_start(buf, sems):
        remote(buf.at[y], buf.at[y], sems.at[0], sems.at[4], {"y": above}).start()
        remote(buf.at[y], buf.at[y], sems.at[1], sems.at[5], {"y": below}).start()

    def ring_forward(buf, sems):
        half = buf.shape[1] // 2
        await_bytes(buf.at[below], sems.at[4])
        low = buf.at[below, pl.ds(0, half)]
        remote(low, low, sems.at[2], sems.at[6], {"y": above}).start()
        await_bytes(buf.at[above], sems.at[5])
        high = buf.at[above, pl.ds(half, half)]
        remote(high, high, sems.at[3], sems.at[7], {"y": below}).start()

    def ring_finish(buf, sems):
        half = buf.shape[1] // 2
        await_bytes(buf.at[far, pl.ds(0, half)], sems.at[6])
        await_bytes(buf.at[far, pl.ds(half, half)], sems.at[7])

    def ring_drain(buf, sems):
        half = buf.shape[1] // 2
        await_bytes(buf.at[y], sems.at[0])
        await_bytes(buf.at[y], sems.at[1])
        await_bytes(buf.at[y, pl.ds(0, half)], sems.at[2])
        await_bytes(buf.at[y, pl.ds(0, half)], sems.at[3])

    def spread_along_y(buf, number):
        for k in range(1, ys):
            to = lax.rem(y + k, ys)
            remote(buf.at[y], buf.at[y], send.at[number], recv.at[number], {"y": to}).start()

    def to_columns(src_at, dst_at, number, to_y=None):
        def one(step, carry):
            pz, px = peer_at(step, z, x, zs, xs)
            to = {"z": pz, "x": px}
            if to_y is not None:
                to["y"] = to_y
            remote(src_at(pz * xs + px), dst_at, send.at[number], recv.at[number], to).start()
            return carry

        lax.fori_loop(0, others, one, 0)

    for k in range(1, 4):
        pz = lax.rem(z + k * fourth, zs)
        own = sh.at[q, r, x, c]
        remote(own, own, send.at[0], recv.at[0], {"z": pz}).start()
    spread_along_y(own_tok, 5)
    to_columns(lambda e: tok_src.at[e], tok_in.at[me], 1)
    to_columns(lambda e: gu_src.at[e], gu.at[me, c], 3)
    share = experts // ys
    down_at = dd.at[y * share + lax.rem(z, part_z) * xs + x, c]

    @pl.when(owner == y)
    def _():
        pltpu.make_async_copy(down_src.at[me], down_at, recv.at[4]).start()

    @pl.when(owner != y)
    def _():
        remote(down_src.at[me], down_at, send.at[9], recv.at[4], {"y": owner}).start()

    to_columns(lambda e: down_src.at[e], down_at, 4, owner)
    await_bytes(sh.at[pl.ds(0, 3), r, x, c], recv.at[0])
    line = sh.at[:, r, x, c]
    for k in range(1, fourth):
        pz = q * fourth + (r + k) % fourth
        remote(line, line, send.at[2], recv.at[2], {"z": pz}).start()
    for k in range(1, xs):
        remote(line, line, send.at[14], recv.at[14], {"x": lax.rem(x + k, xs)}).start()

    await_bytes(tok_in.at[pl.ds(0, others)], recv.at[1])
    group = 8 * CAP
    for g in range(experts // 8):
        lines = tok_in[pl.ds(8 * g, 8)].reshape(8 * slab, LANES)
        turned = jnp.dot(turn[...], lines, preferred_element_type=F32).astype(BF)
        for k in range(4):
            rows[y, pl.ds(g * group, group), pl.ds(k * LANES, LANES)] = turned[
                k * group : (k + 1) * group
            ]
    ring_start(rows, row_sem)
    await_bytes(sh.at[:, r, pl.ds(0, xs - 1), c], recv.at[14])
    first_lines = sh.at[:, r, :, c]
    remote(first_lines, first_lines, send.at[6], recv.at[6], {"c": 1 - c}).start()

    await_bytes(own_tok.at[pl.ds(0, ys - 1)], recv.at[5])
    wide = [own_tok[k].astype(F32) for k in range(ys)]
    total = sum(jnp.sum(w * w, axis=1, keepdims=True) for w in wide)
    factor = lax.rsqrt(total * (1.0 / (ys * tok.shape[1])) + EPS)
    own_normed = [(w * factor).astype(BF) for w in wide]

    ring_forward(rows, row_sem)

    ring_finish(rows, row_sem)
    row_total = jnp.zeros((rows.shape[1], 1), F32)
    for k in range(ys):
        part = rows[k].astype(F32)
        row_total = row_total + jnp.sum(part * part, axis=1, keepdims=True)
    row_factor = lax.rsqrt(row_total * (1.0 / (ys * tok.shape[1])) + EPS)
    for k in range(ys):
        normed[k] = (rows[k].astype(F32) * row_factor).astype(BF)

    nt = (((1,), (1,)), ((), ()))

    def shared_rows(k, number):
        return sh[k, :, :, :, number].reshape(share * 2 * 16, LANES)

    def stacked(ref, k, number):
        return ref[pl.ds(k * share, share), :, number].reshape(share * 2 * 16, LANES)

    await_bytes(gu.at[pl.ds(0, others), c], recv.at[3])
    remote(gu.at[:, c], gu.at[:, c], send.at[8], recv.at[8], {"c": 1 - c}).start()
    await_bytes(gu.at[:, c], recv.at[8])
    act = sum(
        jnp.dot(normed[k], stacked(gu, k, 0), preferred_element_type=F32) for k in range(ys)
    )
    lin = sum(
        jnp.dot(normed[k], stacked(gu, k, 1), preferred_element_type=F32) for k in range(ys)
    )
    hid[y] = (act / (1.0 + jnp.exp(-act)) * lin).astype(BF)
    spread_along_y(hid, 12)

    half_rows = lax.broadcasted_iota(jnp.int32, (64, LANES), 0) + 64 * c
    pick = (half_rows == lax.broadcasted_iota(jnp.int32, (64, LANES), 1)).astype(BF)
    wide_share = share * 2 * 16
    for k in range(ys):
        cols = pl.ds(k * wide_share, wide_share)
        gate_out[0, :, cols] = lax.dot_general(
            pick, stacked(gu, k, 0), nt, preferred_element_type=F32
        ).astype(BF)
        up_out[0, :, cols] = lax.dot_general(
            pick, stacked(gu, k, 1), nt, preferred_element_type=F32
        ).astype(BF)
    stores = [
        pltpu.make_async_copy(src, dst, store_sem.at[number])
        for number, (src, dst) in enumerate((
            (gate_out, gate_hbm_out), (up_out, up_hbm_out), (down_out, down_hbm_out),
            (sg_out, sg_hbm_out), (su_out, su_hbm_out), (sd_out, sd_hbm_out),
            (mixed, mixed_hbm),
        ))
    ]
    for store in stores[:2]:
        store.start()

    await_bytes(dd.at[:, c], recv.at[4])
    remote(dd.at[:, c], dd.at[:, c], send.at[10], recv.at[10], {"c": 1 - c}).start()
    await_bytes(hid.at[pl.ds(0, ys - 1)], recv.at[12])
    await_bytes(dd.at[:, c], recv.at[10])
    result[...] = sum(
        lax.dot_general(
            hid[k], dd[pl.ds(k * share, share)].reshape(wide_share, LANES), nt,
            preferred_element_type=F32,
        )
        for k in range(ys)
    ).astype(BF)

    await_bytes(sh.at[:, pl.ds(0, fourth - 1), x, c], recv.at[2])
    for k in range(1, xs):
        for j in range(1, fourth):
            line = sh.at[:, (r + j) % fourth, x, c]
            to = {"x": lax.rem(x + k, xs)}
            remote(line, line, send.at[13], recv.at[14 + k], to).start()

    def to_other_core(px):
        for j in range(1, fourth):
            line = sh.at[:, (r + j) % fourth, px, c]
            remote(line, line, send.at[6], recv.at[6], {"c": 1 - c}).start()

    to_other_core(x)

    groups = experts // 8

    def send_back(g, count):
        def one(step, carry):
            pz = lax.rem(2 * g + (step // xs) + (z + 1) % 2, 2) + 2 * g
            px = lax.rem(x + 1 + lax.rem(step, xs), xs)
            remote(
                back_src.at[pz * xs + px], back_in.at[me], send.at[11], recv.at[11],
                {"z": pz, "x": px},
            ).start()
            return carry

        lax.fori_loop(0, count, one, 0)

    previous = None
    for offset in (4, 3, 5, 2, 6, 1, 7, 0):
        g = lax.rem(z // 2 + offset, groups)
        part = result[pl.ds(pl.multiple_of(g * group, 16), group), :]
        lines = jnp.concatenate([part[:, k * LANES : (k + 1) * LANES] for k in range(4)], axis=0)
        turned = jnp.dot(turn_back[...], lines, preferred_element_type=F32).astype(BF)
        back_src[pl.ds(8 * g, 8)] = turned.reshape(8, slab, LANES)
        if previous is not None:
            send_back(previous, 8)
        previous = g
    back_in[me] = back_src[me]
    send_back(previous, 7)

    for k in range(ys // 2):
        left = dd[pl.ds(2 * k * share, share)].reshape(wide_share, LANES)
        right = dd[pl.ds((2 * k + 1) * share, share)].reshape(wide_share, LANES)
        left = lax.dot_general(left, pick, nt, preferred_element_type=F32)
        right = lax.dot_general(right, pick, nt, preferred_element_type=F32)
        down_out[0, :, pl.ds(k * LANES, LANES)] = jnp.concatenate([left, right], axis=1).astype(BF)
    stores[2].start()
    for k in (1, 3, 2):
        await_bytes(sh.at[:, pl.ds(0, fourth - 1), x, c], recv.at[14 + k])
        to_other_core(lax.rem(x + xs - k, xs))
    await_bytes(sh.at[:, :, :, c], recv.at[6])
    act = sum(
        jnp.dot(own_normed[k], shared_rows(k, 0), preferred_element_type=F32) for k in range(ys)
    )
    lin = sum(
        jnp.dot(own_normed[k], shared_rows(k, 1), preferred_element_type=F32) for k in range(ys)
    )
    shared_hidden = (act / (1.0 + jnp.exp(-act)) * lin).astype(BF)
    for k in range(ys):
        part_src[k] = lax.dot_general(
            shared_hidden, shared_rows(k, 2), nt, preferred_element_type=F32
        ).astype(BF)
    part_in[y] = part_src[y]
    for k in range(1, ys):
        to = lax.rem(y + k, ys)
        remote(part_src.at[to], part_in.at[y], send.at[7], recv.at[7], {"y": to}).start()

    same = (
        lax.broadcasted_iota(jnp.int32, (LANES, LANES), 0)
        == lax.broadcasted_iota(jnp.int32, (LANES, LANES), 1)
    ).astype(BF)
    for k in range(ys):
        cols = pl.ds(k * wide_share, wide_share)
        sd_out[:, cols] = lax.dot_general(
            same, shared_rows(k, 2), nt, preferred_element_type=F32
        ).astype(BF)
        sg_out[cols, :] = shared_rows(k, 0)
        su_out[cols, :] = shared_rows(k, 1)
    for store in stores[3:-1]:
        store.start()

    await_bytes(part_in.at[pl.ds(0, ys - 1)], recv.at[7])
    shared_sum = sum(part_in[k].astype(F32) for k in range(ys))
    by_slot = jnp.where(first, weight[0:1, :].reshape(1, 1, LANES), 0.0) + jnp.where(
        second, weight[1:2, :].reshape(1, 1, LANES), 0.0
    )
    by_slot = jnp.where(position == slot_f, by_slot.reshape(experts * slab, LANES), 0.0)
    high = by_slot.astype(BF)
    low = (by_slot - high.astype(F32)).astype(BF)
    none = jnp.zeros_like(high)
    tn = (((0,), (0,)), ((), ()))
    await_bytes(back_in.at[pl.ds(0, others)], recv.at[11])
    arrived = back_in[...].reshape(experts * slab, LANES)
    for k in range(4):
        here = block_2d == k
        routed = lax.dot_general(
            jnp.where(here, high, none), arrived, tn, preferred_element_type=F32
        ) + lax.dot_general(jnp.where(here, low, none), arrived, tn, preferred_element_type=F32)
        lanes = slice(k * LANES, (k + 1) * LANES)
        mixed[:, lanes] = (shared_sum[:, lanes] + routed).astype(BF)

    stores[-1].start()

    await_bytes(sh.at[pl.ds(0, 3), r, x, c], send.at[0])
    await_bytes(tok_src.at[pl.ds(0, others)], send.at[1])
    await_bytes(sh.at[:, pl.ds(0, fourth - 1), x, c], send.at[2])
    await_bytes(sh.at[:, r, pl.ds(0, xs - 1), c], send.at[14])
    await_bytes(gu_src.at[pl.ds(0, others)], send.at[3])
    await_bytes(down_src.at[pl.ds(0, others)], send.at[4])
    await_bytes(own_tok.at[pl.ds(0, ys - 1)], send.at[5])
    await_bytes(hid.at[pl.ds(0, ys - 1)], send.at[12])
    await_bytes(sh.at[:, pl.ds(0, fourth - 1), pl.ds(0, xs - 1), c], send.at[13])
    await_bytes(sh.at[:, :, :, c], send.at[6])
    await_bytes(part_src.at[pl.ds(0, ys - 1)], send.at[7])
    await_bytes(gu.at[:, c], send.at[8])

    @pl.when(owner != y)
    def _():
        await_bytes(down_src.at[me], send.at[9])

    await_bytes(dd.at[:, c], send.at[10])
    await_bytes(back_src.at[pl.ds(0, others)], send.at[11])
    ring_drain(rows, row_sem)
    for store in stores:
        store.wait()


def write_out(*refs):
    sources, targets, held, sems = refs[:7], refs[7:14], refs[14:21], refs[21]
    into = [pltpu.make_async_copy(sources[k], held[k], sems.at[k]) for k in range(7)]
    out = [pltpu.make_async_copy(held[k], targets[k], sems.at[7 + k]) for k in range(7)]
    for copy in into:
        copy.start()
    for k in range(7):
        into[k].wait()
        out[k].start()
    for copy in out:
        copy.wait()


def on_device(zs, xs, ys, tokens, routes, route_weight, norm_gain, e_gate, e_up, e_down, s_gate, s_up, s_down):
    experts, d_rows, _ = e_gate.shape
    tok_count, width = tokens.shape
    slab = 4 * CAP
    turn = turn_matrix()
    all_rows = experts * CAP
    model = experts * 2 * d_rows
    hbm = pl.BlockSpec(memory_space=pltpu.HBM)
    made = (
        ((tok_count, width), BF),
        ((1, 64, model), BF),
        ((1, 64, model), BF),
        ((1, width, 2 * LANES), BF),
        ((model, LANES), BF),
        ((model, LANES), BF),
        ((LANES, model), BF),
    )
    outs = pl.pallas_call(
        functools.partial(kernel, zs, xs, ys),
        out_shape=tuple(jax.ShapeDtypeStruct(*m) for m in made),
        in_specs=[hbm] * 12,
        out_specs=(hbm,) * 7,
        scratch_shapes=[pltpu.VMEM(*m) for m in made]
        + [
            pltpu.VMEM((experts, slab, LANES), BF),
            pltpu.VMEM((experts, 2, d_rows, LANES), BF),
            pltpu.VMEM((experts, d_rows, LANES), BF),
            pltpu.VMEM((experts, slab, LANES), BF),
            pltpu.VMEM((experts, 2, 2, d_rows, LANES), BF),
            pltpu.VMEM((experts, 2, d_rows, LANES), BF),
            pltpu.VMEM((4, zs // 4, xs, 2, 3, d_rows, LANES), BF),
            pltpu.VMEM((ys, tok_count, width), BF),
            pltpu.VMEM((ys, all_rows, width), BF),
            pltpu.VMEM((ys, all_rows, width), BF),
            pltpu.VMEM((ys, all_rows, LANES), BF),
            pltpu.VMEM((ys, tok_count, width), BF),
            pltpu.VMEM((ys, tok_count, width), BF),
            pltpu.VMEM((all_rows, width), BF),
            pltpu.VMEM((experts, slab, LANES), BF),
            pltpu.VMEM((experts, slab, LANES), BF),
            pltpu.VMEM((tok_count, width), BF),
            pltpu.VMEM((2, LANES), jnp.int32),
            pltpu.VMEM((2, LANES), F32),
            pltpu.VMEM((d_rows,), F32),
            pltpu.VMEM((experts, d_rows, LANES), F32),
            pltpu.VMEM((experts, d_rows, LANES), F32),
            pltpu.VMEM((experts, d_rows, LANES), F32),
            pltpu.VMEM((d_rows, LANES), F32),
            pltpu.VMEM((d_rows, LANES), F32),
            pltpu.VMEM((d_rows, LANES), F32),
            pltpu.VMEM(turn.shape, BF),
            pltpu.VMEM(turn.shape, BF),
            pltpu.SemaphoreType.DMA((15,)),
            pltpu.SemaphoreType.DMA((18,)),
            pltpu.SemaphoreType.DMA((8,)),
            pltpu.SemaphoreType.DMA((12,)),
            pltpu.SemaphoreType.DMA((7,)),
        ],
        compiler_params=pltpu.CompilerParams(
            collective_id=0, has_side_effects=True, vmem_limit_bytes=61000 * 1024
        ),
    )(
        tokens, routes.T, route_weight.T, norm_gain, e_gate, e_up, e_down, s_gate, s_up, s_down.T,
        jnp.asarray(turn, BF), jnp.asarray(turn.T, BF),
    )
    mixed, gate_t, up_t, down_new, sg, su, sd = pl.pallas_call(
        write_out,
        out_shape=tuple(jax.ShapeDtypeStruct(o.shape, o.dtype) for o in outs),
        in_specs=[hbm] * 7,
        out_specs=(hbm,) * 7,
        scratch_shapes=[pltpu.VMEM(*m) for m in made] + [pltpu.SemaphoreType.DMA((14,))],
        compiler_params=pltpu.CompilerParams(vmem_limit_bytes=61000 * 1024),
    )(*outs)
    return (
        mixed, gate_t.transpose(0, 2, 1), up_t.transpose(0, 2, 1), down_new, sg, su, sd,
    )


def solution(mesh):
    tp = mesh.shape["tp"]
    devices = mesh.devices.reshape(16, 4, 2, tp)
    split = Mesh(devices, ("z", "x", "c", "y"))
    zs, xs, _, ys = devices.shape
    placed = (
        P(FS, "y"),
        P(FS, None),
        P(FS, None),
        P(FS),
        P(None, FS, "y"),
        P(None, FS, "y"),
        P(None, FS, "y"),
        P(FS, "y"),
        P(FS, "y"),
        P("y", FS),
    )
    return jax.shard_map(
        functools.partial(on_device, zs, xs, ys),
        mesh=split,
        in_specs=placed,
        out_specs=(
            P(FS, "y"),
            P(FS, None, "y"),
            P(FS, None, "y"),
            P(FS, "y", None),
            P(None, "y"),
            P(None, "y"),
            P("y", None),
        ),
        check_vma=False,
    )
```
